512 devices in a mesh: grp: 2 (over y), fs: 32 (over z), tp: 8 (over x, core).
Axes of the slice: x: 4, y: 2, z: 32, core: 2. Of those that a mesh axis runs over, the one named last changes fastest.
The devices are a block of a 4x8x32 slice.
Arguments:
- tokens: bfloat16 [24576, 2048], P(('grp', 'fs'), 'tp'), parts along dimension 0, may hold values from -6 to 6
- mix_gain: float32 [2048], replicated, may hold values from 0.1 to 1.9
- w_signal: bfloat16 [2048, 1024], P('fs', 'tp'), may hold values from -0.125 to 0.125
- w_outer_gate: bfloat16 [2048, 1024], P('fs', 'tp'), may hold values from -0.125 to 0.125
- w_inner_gate: bfloat16 [2048, 1024], P('fs', 'tp'), may hold values from -0.125 to 0.125
- mix_taps: float32 [3, 1024], P(None, 'tp'), may hold values from -3 to 3
- w_mix_out: bfloat16 [1024, 2048], P('tp', 'fs'), may hold values from -0.1875 to 0.1875
- ffn_gain: float32 [2048], replicated, may hold values from 0.1 to 1.9
- w_gate: bfloat16 [2048, 5120], P('fs', 'tp'), may hold values from -0.125 to 0.125
- w_value: bfloat16 [2048, 5120], P('fs', 'tp'), may hold values from -0.125 to 0.125
- up_taps: float32 [2, 3, 5120], P(None, None, 'tp'), may hold values from -3 to 3
- up_bias: float32 [2, 5120], P(None, 'tp'), may hold values from -3 to 3
- w_down: bfloat16 [5120, 2048], P('tp', 'fs'), may hold values from -0.078125 to 0.078125
Outputs:
- layer_out: bfloat16 [24576, 2048], P(('grp', 'fs'), 'tp'), parts along dimension 0
The draws below stay inside these ranges and needn't reach their ends.
There are 2 independent parts, one for each index of `grp`. The reference program is written for one: setup_inputs(seed, part) draws one part's arguments, and reference() takes and returns one part's arrays. A program takes and returns all parts, laid end to end along the dimension named above; an argument that names none is the same for every part. Nothing has to cross between parts.
All inputs are finite; a program needn't handle non-finite values.
Results may differ from the reference program's by a relative error of at most 0.022.
Values may be sent and summed in bfloat16 or wider, within the bound.
A program may use at most 64 MiB of HBM per device.

```python
import jax
import jax.numpy as jnp
from jax import lax

D = 2048
DC = 1024
FF = 5120
TAPS = 3
LEN = 192
TOKENS = 12288
N_TP = 8


def block_levels(stream_key, extent, split, least, high):
    level, own = 1.0, jax.random.fold_in(stream_key, 6)
    for dim, blocks in split:
        steps = jnp.exp(jax.random.uniform(jax.random.fold_in(own, dim), (blocks,), jnp.float32, least / len(split), high / len(split)))
        level = level * jnp.repeat(steps, extent[dim] // blocks).reshape([-1 if axis == dim else 1 for axis in range(len(extent))])
    return level


def centred(rng, dims, deviation, bound, shards=(), dtype=jnp.bfloat16):
    drawn = jax.random.normal(rng, dims, jnp.float32) * deviation
    if len(shards) > 0:
        drawn = block_levels(rng, dims, shards, -0.22, 0.18) * drawn
    return jnp.clip(drawn, min=-bound, max=bound).astype(dtype)


def setup_inputs(seed: int = 0, part: int = 0) -> dict:
    key_list = jax.random.split(jax.random.key(seed), 14)
    part_splits = jax.random.split(jax.random.fold_in(key_list[13], part), 14)
    return {
        "tokens": centred(part_splits[0], (TOKENS, D), 1.0, 6.0, ((0, 32), (1, 8))),
        "mix_gain": jnp.clip(1.0 + 0.18 * jax.random.normal(key_list[1], (D,), jnp.float32), 0.1, 1.9),
        "w_signal": centred(key_list[2], (D, DC), D ** -0.5, 0.125, ((0, 32), (1, 8))),
        "w_outer_gate": centred(key_list[3], (D, DC), D ** -0.5, 0.125, ((0, 32), (1, 8))),
        "w_inner_gate": centred(key_list[4], (D, DC), D ** -0.5, 0.125, ((0, 32), (1, 8))),
        "mix_taps": centred(key_list[5], (TAPS, DC), 0.577, 3.0, ((1, 8),), jnp.float32),
        "w_mix_out": centred(key_list[6], (DC, D), DC ** -0.5, 0.1875, ((0, 8), (1, 32))),
        "ffn_gain": jnp.clip(1.0 + 0.18 * jax.random.normal(key_list[7], (D,), jnp.float32), 0.1, 1.9),
        "w_gate": centred(key_list[8], (D, FF), D ** -0.5, 0.125, ((0, 32), (1, 8))),
        "w_value": centred(key_list[9], (D, FF), D ** -0.5, 0.125, ((0, 32), (1, 8))),
        "up_taps": centred(key_list[10], (2, TAPS, FF), 0.577, 3.0, ((2, 8),), jnp.float32),
        "up_bias": centred(key_list[11], (2, FF), 0.5, 3.0, ((1, 8),), jnp.float32),
        "w_down": centred(key_list[12], (FF, D), FF ** -0.5, 0.078125, ((0, 8), (1, 32))),
    }


def conv_positions(values, taps):
    width = values.shape[1]
    blocks = values.reshape(-1, LEN, width)
    padded = jnp.pad(blocks, ((0, 0), (2, 0), (0, 0)))
    result = padded[:, 0:LEN] * taps[0] + padded[:, 1:LEN + 1] * taps[1] + padded[:, 2:LEN + 2] * taps[2]
    return result.reshape(-1, width)

def rms_norm(stream, gain):
    values = stream.astype(jnp.float32)
    scale = lax.rsqrt(lax.optimization_barrier(jnp.mean(values * values, axis=-1, keepdims=True)) + 1e-06)
    return (values * scale * gain).astype(jnp.bfloat16)

def block_partials(left, right, blocks):
    width = left.shape[1] // blocks
    total = jnp.zeros((left.shape[0], right.shape[1]), jnp.float32)
    for index in range(blocks):
        part = jnp.dot(left[:, index * width:(index + 1) * width], right[index * width:(index + 1) * width], preferred_element_type=jnp.float32)
        part = lax.optimization_barrier(part.astype(jnp.bfloat16))
        total = total + part.astype(jnp.float32)
    return total

def reference(tokens, mix_gain, w_signal, w_outer_gate, w_inner_gate, mix_taps, w_mix_out, ffn_gain, w_gate, w_value, up_taps, up_bias, w_down):
    normed = rms_norm(tokens, mix_gain)
    signal = jnp.dot(normed, w_signal, preferred_element_type=jnp.float32).astype(jnp.bfloat16)
    outer = jnp.dot(normed, w_outer_gate, preferred_element_type=jnp.float32).astype(jnp.bfloat16)
    inner = jnp.dot(normed, w_inner_gate, preferred_element_type=jnp.float32).astype(jnp.bfloat16)
    product = inner.astype(jnp.float32) * signal.astype(jnp.float32)
    mixed = (outer.astype(jnp.float32) * conv_positions(product, mix_taps)).astype(jnp.bfloat16)
    mix_sum = block_partials(mixed, w_mix_out, N_TP)
    resid = (tokens.astype(jnp.float32) + mix_sum).astype(jnp.bfloat16)
    normed_ffn = rms_norm(resid, ffn_gain)
    gate = jnp.dot(normed_ffn, w_gate, preferred_element_type=jnp.float32).astype(jnp.bfloat16)
    value = jnp.dot(normed_ffn, w_value, preferred_element_type=jnp.float32).astype(jnp.bfloat16)
    gate_conv = conv_positions(gate.astype(jnp.float32), up_taps[0]) + up_bias[0]
    value_conv = conv_positions(value.astype(jnp.float32), up_taps[1]) + up_bias[1]
    hidden = (jax.nn.silu(gate_conv) * value_conv).astype(jnp.bfloat16)
    ffn_sum = block_partials(hidden, w_down, N_TP)
    return (resid.astype(jnp.float32) + ffn_sum).astype(jnp.bfloat16)
```

```python
import functools

import jax
import jax.numpy as jnp
from jax import lax
from jax.experimental import pallas as pl
from jax.experimental.pallas import tpu as pltpu
from jax.sharding import PartitionSpec as P

SEQS_DEV = 2
LANES = 128
MESH = pl.DeviceIdType.MESH
F32, BF16 = jnp.float32, jnp.bfloat16

ONE = {"m": 2, "g": 3, "d": 1}
BOTH = {"m": 0, "g": 4, "d": 3}


def conv_positions(values, taps, length):
    row = lax.rem(lax.broadcasted_iota(jnp.int32, values.shape, 0), length)
    back1 = jnp.where(row >= 1, pltpu.roll(values, 1, 0), 0.0)
    back2 = jnp.where(row >= 2, pltpu.roll(values, 2, 0), 0.0)
    return back2 * taps[0:1] + back1 * taps[1:2] + values * taps[2:3]


def dot(a, b):
    return jnp.dot(a, b, preferred_element_type=F32)


def dot_nt(a, b):
    return lax.dot_general(a, b, (((1,), (1,)), ((), ())), preferred_element_type=F32)


def kernel(
    sizes,
    tok, mix_gain, w_sig, w_out, w_inn, mix_taps, w_mo, ffn_gain, w_gate, w_val, up_taps, up_bias, w_down,
    out,
    gm, gg, gd, act0, act1, normed, terms0, terms1, mate0, mate1, turn0, turn1, fin0, fin1, resid, hidden,
    zs_send, zs_recv, ys_send, ys_recv, ag_send, ag_recv, rs_send, rs_recv,
):
    ngrp, nz, ntp = sizes
    nx = ntp // 2
    rows, db = tok.shape
    half = rows // 2
    length = rows // SEQS_DEV
    depth = w_sig.shape[0]
    g, z, t = lax.axis_index("grp"), lax.axis_index("fs"), lax.axis_index("tp")
    y, x, c = lax.rem(g, 2), lax.div(t, 2), lax.rem(t, 2)
    pair = {"grp": g + 1 - 2 * y}
    xr, xl, x2 = lax.rem(x + 1, nx), lax.rem(x + nx - 1, nx), lax.rem(x + 2, nx)
    x_right, x_left, mate = {"tp": 2 * xr + c}, {"tp": 2 * xl + c}, {"tp": 2 * x + 1 - c}
    z_nbr = ({"fs": lax.rem(z + 1, nz)}, {"fs": lax.rem(z + nz - 1, nz)})

    def remote(src, dst, ssem, rsem, dev):
        return pltpu.make_async_remote_copy(
            src_ref=src, dst_ref=dst, send_sem=ssem, recv_sem=rsem, device_id=dev, device_id_type=MESH
        )

    sets = {"m": (gm, 0), "g": (gg, 1), "d": (gd, 2)}
    steps = (nz // 2, (nz - 1) // 2)

    def piece(ref, first, count, origin):
        return ref.at[pl.ds(first, count), pl.ds(pl.multiple_of(origin * depth, depth), depth), :]

    def origin_of(way, s):
        return lax.rem(z + (nz - s if way == 0 else s), nz)

    def z_copy(name, way, s):
        ref, k = sets[name]
        part = piece(ref, ONE[name] * y, ONE[name] + BOTH[name], origin_of(way, s))
        return remote(part, part, zs_send.at[k, way, s], zs_recv.at[k, way, s], z_nbr[way])

    def z_arrive(name, way, s):
        ref, k = sets[name]
        part = piece(ref, ONE[name] * y, ONE[name] + BOTH[name], origin_of(way, s + 1))
        remote(part, part, zs_send.at[k, way, s], zs_recv.at[k, way, s], z_nbr[way]).wait_recv()

    def y_copy(name, way, s):
        ref, k = sets[name]
        part = piece(ref, (ONE[name] + BOTH[name]) * y, ONE[name], origin_of(way, s + 1))
        return remote(part, part, ys_send.at[k, way, s], ys_recv.at[k], pair)

    def z_open(name):
        for way in (0, 1):
            z_copy(name, way, 0).start()

    def z_step(name, s):
        for way in (0, 1):
            def go(way=way):
                z_arrive(name, way, s)
                pl.when(s + 1 < steps[way])(lambda: z_copy(name, way, s + 1).start())
                y_copy(name, way, s).start()
            pl.when(s < steps[way])(go)

    def z_steps(name, lo, hi):
        def body(s, _):
            z_step(name, s)
            return 0
        lax.fori_loop(lo, hi, body, 0)

    def y_arrive(name):
        ref, k = sets[name]
        part = ref.at[pl.ds(0, ONE[name]), pl.ds(0, (nz - 1) * depth), :]
        remote(part, part, ys_send.at[k, 0, 0], ys_recv.at[k], pair).wait_recv()

    def ag_copies(act, k):
        own, lft, rgt, far = act.at[t], act.at[2 * xl + c], act.at[2 * xr + c], act.at[2 * x2 + c]
        top, bot = pl.ds(0, half), pl.ds(half, half)
        plan = (
            (own, x_right), (own, x_left), (own, mate),
            (lft.at[top], x_right), (lft, mate), (rgt.at[bot], x_left), (rgt, mate),
            (far.at[top], mate), (far.at[bot], mate),
        )
        return [remote(r, r, ag_send.at[k, i], ag_recv.at[k, i], dev) for i, (r, dev) in enumerate(plan)]

    def ag_lands(act, k):
        o = 1 - c
        top, bot = pl.ds(0, half), pl.ds(half, half)
        far, ofar = act.at[2 * x2 + c], act.at[2 * x2 + o]
        plan = (
            act.at[2 * xl + c], act.at[2 * xr + c], act.at[2 * x + o],
            far.at[top], act.at[2 * xl + o], far.at[bot], act.at[2 * xr + o],
            ofar.at[top], ofar.at[bot],
        )
        return [remote(r, r, ag_send.at[k, i], ag_recv.at[k, i], mate) for i, r in enumerate(plan)]

    def rs_copies(k, terms, mt, turn, fin):
        top, bot = pl.ds(0, half), pl.ds(half, half)
        plan = [(terms.at[2 * v + 1 - c], mt.at[v], mate) for v in (x2, xr, xl, x)]
        plan += [
            (terms.at[2 * x2 + c, top], turn.at[0], x_right),
            (terms.at[2 * x2 + c, bot], turn.at[1], x_left),
            (terms.at[2 * xr + c, bot], fin.at[0, bot], x_right),
            (terms.at[2 * xl + c, top], fin.at[1, top], x_left),
            (terms.at[2 * xr + c, top], fin.at[0, top], x_right),
            (terms.at[2 * xl + c, bot], fin.at[1, bot], x_left),
        ]
        return [remote(s, d, rs_send.at[k, i], rs_recv.at[k, i], dev) for i, (s, d, dev) in enumerate(plan)]

    def reduce_scatter(k, term_of, terms, mt, turn, fin, between):
        copies = rs_copies(k, terms, mt, turn, fin)
        top, bot = pl.ds(0, half), pl.ds(half, half)
        for i, v in enumerate((x2, xr, xl, x)):
            terms[2 * v + 1 - c] = term_of(2 * v + 1 - c).astype(BF16)
            copies[i].start()
            terms[2 * v + c] = term_of(2 * v + c).astype(BF16)

        def join(i, v):
            copies[i].wait_recv()
            terms[2 * v + c] = (terms[2 * v + c].astype(F32) + mt[v].astype(F32)).astype(BF16)

        join(0, x2)
        copies[4].start()
        copies[5].start()
        join(1, xr)
        copies[6].start()
        join(2, xl)
        copies[7].start()
        between()
        copies[4].wait_recv()
        terms[2 * xr + c, top] = (terms[2 * xr + c, top].astype(F32) + turn[0].astype(F32)).astype(BF16)
        copies[8].start()
        copies[5].wait_recv()
        terms[2 * xl + c, bot] = (terms[2 * xl + c, bot].astype(F32) + turn[1].astype(F32)).astype(BF16)
        copies[9].start()
        copies[3].wait_recv()
        total = terms[2 * x + c].astype(F32) + mt[x].astype(F32)
        for i in (6, 7, 8, 9):
            copies[i].wait_recv()
        total += fin[0].astype(F32) + fin[1].astype(F32)
        return total, copies

    def norm(act, gain):
        total = jnp.zeros((rows, 1), F32)
        for b in range(ntp):
            v = act[b].astype(F32)
            total += jnp.sum(v * v, axis=1, keepdims=True)
        scale = lax.rsqrt(total / (ntp * db) + 1e-06)
        for b in range(ntp):
            cols = slice(b * db, (b + 1) * db)
            normed[:, cols] = (act[b].astype(F32) * scale * gain[:, cols]).astype(BF16)

    mine = pl.ds(pl.multiple_of(z * depth, depth), depth)
    eye = (
        lax.broadcasted_iota(jnp.int32, (depth, depth), 0) == lax.broadcasted_iota(jnp.int32, (depth, depth), 1)
    ).astype(BF16)
    for k, ref in enumerate((w_sig, w_out, w_inn)):
        gm[k, mine, :] = ref[...]
    gm[3, mine, :] = dot_nt(eye, w_mo[...]).astype(BF16)
    act0[t] = tok[...]
    nf = w_gate.shape[1] // LANES
    for b in range(nf):
        cols = slice(b * LANES, (b + 1) * LANES)
        gg[b, mine, :] = w_gate[:, cols]
        gg[nf + b, mine, :] = w_val[:, cols]
        gd[b, mine, :] = dot_nt(eye, w_down[cols, :]).astype(BF16)

    barrier = pltpu.get_barrier_semaphore()
    friends = (x_right, x_left, mate, *z_nbr, pair)
    for dev in friends:
        pl.semaphore_signal(barrier, inc=1, device_id=dev, device_id_type=MESH)
    pl.semaphore_wait(barrier, len(friends))

    z_open("m")
    ag0, land0 = ag_copies(act0, 0), ag_lands(act0, 0)
    for i in (0, 1, 2):
        ag0[i].start()
    z_open("g")

    z_step("m", 0)
    land0[0].wait_recv()
    ag0[3].start()
    ag0[4].start()
    land0[1].wait_recv()
    ag0[5].start()
    ag0[6].start()
    z_step("m", 1)
    z_step("g", 0)
    z_step("m", 2)
    land0[3].wait_recv()
    ag0[7].start()
    land0[5].wait_recv()
    ag0[8].start()
    z_step("m", 3)
    z_step("g", 1)
    z_step("m", 4)
    for i in (2, 4, 6, 7, 8):
        land0[i].wait_recv()
    norm(act0, mix_gain)

    last = steps[0]

    def pace(i, _):
        z_step("m", 2 * i + 1)
        z_step("g", i)
        z_step("m", 2 * i + 2)
        return 0

    lax.fori_loop(2, (last - 1) // 2, pace, 0)
    z_step("m", last - 1)
    done_g = (last - 1) // 2
    z_step("g", done_g)
    y_arrive("m")

    three = dot(normed[...], jnp.concatenate([gm[0], gm[1], gm[2]], axis=1)).astype(BF16).astype(F32)
    signal, outer, inner = (three[:, k * LANES : (k + 1) * LANES] for k in range(3))
    mixed = (outer * conv_positions(inner * signal, mix_taps[...], length)).astype(BF16)
    z_step("g", done_g + 1)

    def mix_term(b):
        return dot_nt(mixed, gm[3, pl.ds(pl.multiple_of(b * db, db), db), :])

    total, rs0 = reduce_scatter(0, mix_term, terms0, mate0, turn0, fin0, lambda: z_steps("g", done_g + 2, done_g + 4))
    stream = (tok[...].astype(F32) + total).astype(BF16)
    resid[...] = stream
    act1[t] = stream
    ag1, land1 = ag_copies(act1, 1), ag_lands(act1, 1)
    for i in (0, 1, 2):
        ag1[i].start()
    z_open("d")
    z_step("g", done_g + 4)
    land1[0].wait_recv()
    ag1[3].start()
    ag1[4].start()
    land1[1].wait_recv()
    ag1[5].start()
    ag1[6].start()
    z_step("g", done_g + 5)
    land1[3].wait_recv()
    ag1[7].start()
    land1[5].wait_recv()
    ag1[8].start()
    for i in (2, 4, 6, 7, 8):
        land1[i].wait_recv()
    norm(act1, ffn_gain)
    z_steps("g", done_g + 6, last)

    def d_pace(s, _):
        z_step("d", s)
        return 0

    lax.fori_loop(0, 2, d_pace, 0)
    y_arrive("g")
    for b in range(nf):
        both = dot(normed[...], jnp.concatenate([gg[b], gg[nf + b]], axis=1)).astype(BF16).astype(F32)
        cols = slice(b * LANES, (b + 1) * LANES)
        gate = conv_positions(both[:, :LANES], up_taps[0, :, cols], length) + up_bias[0:1, cols]
        value = conv_positions(both[:, LANES:], up_taps[1, :, cols], length) + up_bias[1:2, cols]
        hidden[:, cols] = (gate / (1.0 + jnp.exp(-gate)) * value).astype(BF16)
        z_step("d", 2 + b)
    lax.fori_loop(2 + nf, last, d_pace, 0)
    y_arrive("d")

    def ffn_term(b):
        at = pl.ds(pl.multiple_of(b * db, db), db)
        return dot_nt(hidden[...], jnp.concatenate([gd[i, at, :] for i in range(nf)], axis=1))

    total, rs1 = reduce_scatter(1, ffn_term, terms1, mate1, turn1, fin1, lambda: None)
    out[...] = (resid[...].astype(F32) + total).astype(BF16)

    for copy in (*ag0, *ag1, *rs0, *rs1):
        copy.wait_send()
    for name in sets:
        for way in (0, 1):
            def drain(s, _, name=name, way=way):
                z_copy(name, way, s).wait_send()
                y_copy(name, way, s).wait_send()
                return 0
            lax.fori_loop(0, steps[way], drain, 0)


def on_device(sizes, tokens, mix_gain, w_signal, w_outer, w_inner, mix_taps, w_mix_out, ffn_gain, w_gate, w_value, up_taps, up_bias, w_down):
    rows, db = tokens.shape
    ntp, nz = sizes[2], sizes[1]
    d = ntp * db
    nf = w_gate.shape[1] // LANES
    half = rows // 2
    vmem, dma = pltpu.VMEM, pltpu.SemaphoreType.DMA
    act = vmem((ntp, rows, db), BF16)
    mt, turn, fin = vmem((ntp // 2, rows, db), BF16), vmem((2, half, db), BF16), vmem((2, rows, db), BF16)
    scratch = [
        vmem((4, d, LANES), BF16), vmem((2 * nf, d, LANES), BF16), vmem((nf, d, LANES), BF16),
        act, act, vmem((rows, d), BF16), act, act, mt, mt, turn, turn, fin, fin,
        vmem((rows, db), BF16), vmem((rows, nf * LANES), BF16),
        dma((3, 2, nz // 2)), dma((3, 2, nz // 2)), dma((3, 2, nz // 2)), dma((3,)),
        dma((2, 9)), dma((2, 9)), dma((2, 10)), dma((2, 10)),
    ]
    args = (
        tokens, mix_gain.reshape(1, d), w_signal, w_outer, w_inner, mix_taps, w_mix_out, ffn_gain.reshape(1, d),
        w_gate, w_value, up_taps, up_bias, w_down,
    )
    return pl.pallas_call(
        functools.partial(kernel, sizes),
        out_shape=jax.ShapeDtypeStruct((rows, db), BF16),
        in_specs=[pl.BlockSpec(memory_space=vmem)] * len(args),
        out_specs=pl.BlockSpec(memory_space=vmem),
        scratch_shapes=scratch,
        compiler_params=pltpu.CompilerParams(
            collective_id=0, has_side_effects=True, vmem_limit_bytes=60 * 1024 * 1024
        ),
        name="layer",
    )(*args)


def solution(mesh):
    sizes = (mesh.shape["grp"], mesh.shape["fs"], mesh.shape["tp"])
    placed = (
        P(("grp", "fs"), "tp"), P(), P("fs", "tp"), P("fs", "tp"), P("fs", "tp"), P(None, "tp"), P("tp", "fs"), P(),
        P("fs", "tp"), P("fs", "tp"), P(None, None, "tp"), P(None, "tp"), P("tp", "fs"),
    )
    return jax.shard_map(
        functools.partial(on_device, sizes),
        mesh=mesh, in_specs=placed, out_specs=P(("grp", "fs"), "tp"), check_vma=False,
    )
```

```python
import functools

import jax
import jax.numpy as jnp
from jax import lax
from jax.experimental import pallas as pl
from jax.experimental.pallas import tpu as pltpu
from jax.sharding import PartitionSpec as P

SEQS_DEV = 2
LANES = 128
MESH = pl.DeviceIdType.MESH
F32, BF16 = jnp.float32, jnp.bfloat16

ONE = {"m": 2, "g": 4, "d": 1}
BOTH = {"m": 0, "g": 2, "d": 3}
UP_M, UP_F = 16, 16
MIXER_AT = 8


def conv_positions(values, taps, length):
    row = lax.rem(lax.broadcasted_iota(jnp.int32, values.shape, 0), length)
    back1 = jnp.where(row >= 1, pltpu.roll(values, 1, 0), 0.0)
    back2 = jnp.where(row >= 2, pltpu.roll(values, 2, 0), 0.0)
    return back2 * taps[0:1] + back1 * taps[1:2] + values * taps[2:3]


def dot(a, b):
    return jnp.dot(a, b, preferred_element_type=F32)


def dot_nt(a, b):
    return lax.dot_general(a, b, (((1,), (1,)), ((), ())), preferred_element_type=F32)


def kernel(
    sizes,
    tok, mix_gain, w_sig, w_out, w_inn, mix_taps, w_mo, ffn_gain, w_gate, w_val, up_taps, up_bias, w_down,
    out,
    gm, gg, gd, act0, act1, normed, terms0, terms1, mate0, mate1, turn0, turn1, fin0, fin1, resid, hidden,
    m_recv, g_recv, d_recv, ring_send, y_send, y_recv, push_send, push_recv, own_send, own_recv,
    ag_send, ag_recv, rs_send, rs_recv,
):
    ngrp, nz, ntp = sizes
    nx = ntp // 2
    rows, db = tok.shape
    half = rows // 2
    length = rows // SEQS_DEV
    depth = w_sig.shape[0]
    nf = w_gate.shape[1] // LANES
    g, z, t = lax.axis_index("grp"), lax.axis_index("fs"), lax.axis_index("tp")
    y, x, c = lax.rem(g, 2), lax.div(t, 2), lax.rem(t, 2)
    other = g + 1 - 2 * y
    xr, xl, x2 = lax.rem(x + 1, nx), lax.rem(x + nx - 1, nx), lax.rem(x + 2, nx)
    x_right, x_left, mate = {"tp": 2 * xr + c}, {"tp": 2 * xl + c}, {"tp": 2 * x + 1 - c}
    def remote(src, dst, ssem, rsem, dev):
        return pltpu.make_async_remote_copy(
            src_ref=src, dst_ref=dst, send_sem=ssem, recv_sem=rsem, device_id=dev, device_id_type=MESH
        )

    refs = {"m": gm, "g": gg, "d": gd}
    index = {"m": 0, "g": 1, "d": 2}
    most = {"m": (UP_M, nz - 1 - UP_M), "g": (UP_F, nz - 1 - UP_F), "d": (UP_F, nz - 1 - UP_F)}
    recv_of = {"m": m_recv, "g": g_recv, "d": d_recv}
    is_m, is_f = c == 1, c == 0

    def z_part(name, col, origin):
        at = pl.ds(pl.multiple_of(origin * depth, depth), depth)
        return refs[name].at[col, pl.ds(ONE[name] * y, ONE[name] + BOTH[name]), at, :]

    def y_part(name, col, origin):
        at = pl.ds(pl.multiple_of(origin * depth, depth), depth)
        return refs[name].at[col, pl.ds((ONE[name] + BOTH[name]) * y, ONE[name]), at, :]

    def fs_at(k):
        return lax.rem(z + nz + k, nz)

    def origin_of(way, dist):
        return fs_at(-dist if way == 0 else dist)

    def send(name, col, way, dist, hops):
        part = z_part(name, col, origin_of(way, dist))
        to = {"fs": fs_at(hops if way == 0 else -hops)}
        remote(part, part, ring_send.at[index[name]], recv_of[name].at[col, way, dist + hops - 1], to).start()

    def landed(name, col, way, dist):
        part = z_part(name, col, origin_of(way, dist))
        sem = recv_of[name].at[col, way, dist - 1]
        remote(part, part, ring_send.at[index[name]], sem, mate).wait_recv()

    def spread(name, col, way, dist):
        k, origin = index[name], origin_of(way, dist)
        part, cross = z_part(name, col, origin), y_part(name, col, origin)
        remote(cross, cross, y_send.at[k], y_recv.at[k], {"grp": other, "tp": 2 * x + col}).start()
        if col != (1 if name == "m" else 0):
            remote(part, part, push_send.at[k], push_recv.at[k], mate).start()

    def mixer_step(way, first, upto):
        for dist in (first, first + 1):
            @pl.when(dist <= upto)
            def _(dist=dist):
                for col in (0, 1):
                    landed("m", col, way, dist)
                    pl.when(dist + 2 <= upto)(lambda: send("m", col, way, dist, 2))
                for col in (0, 1):
                    spread("m", col, way, dist)

    def bulk_step(i):
        dist = i + 1
        for col in (0, 1):
            for name in ("g", "d"):
                for way in (0, 1):
                    @pl.when(dist <= most[name][way])
                    def _(way=way):
                        landed(name, col, way, dist)
                        pl.when(dist + 1 <= most[name][way])(lambda: send(name, col, way, dist, 1))
                        spread(name, col, way, dist)

    def open_ring(kind, cols):
        for col in cols:
            for way in (0, 1):
                if kind == "m":
                    send("m", col, way, 0, 1)
                    send("m", col, way, 0, 2)
                else:
                    for name in ("g", "d"):
                        send(name, col, way, 0, 1)

    mixer_end = (max(most["m"]) + 1) // 2
    bulk_end = max(most["g"])

    def mixer_steps(lo, hi):
        def body(i, _):
            for way in (0, 1):
                mixer_step(way, 2 * i + 1, most["m"][way])
            return 0

        lax.fori_loop(lo, jnp.where(is_m, hi, lo), body, 0)

    def bulk_steps(lo, hi):
        hi = min(hi, bulk_end)
        lax.fori_loop(lo, jnp.where(is_f, hi, lo), lambda i, _: (bulk_step(i), 0)[1], 0)
        return hi

    def arrive(name):
        k, span = index[name], pl.ds(0, (nz - 1) * depth)
        part = refs[name].at[0, pl.ds(0, ONE[name]), span, :]
        remote(part, part, y_send.at[k], y_recv.at[k], mate).wait_recv()
        rest = refs[name].at[0, pl.ds(0, ONE[name] + BOTH[name]), span, :]
        pl.when(is_f if name == "m" else is_m)(
            lambda: remote(rest, rest, push_send.at[k], push_recv.at[k], mate).wait_recv()
        )

    def ag_copies(act, k):
        own, lft, rgt, far = act.at[t], act.at[2 * xl + c], act.at[2 * xr + c], act.at[2 * x2 + c]
        top, bot = pl.ds(0, half), pl.ds(half, half)
        plan = (
            (own, x_right), (own, x_left), (own, mate),
            (lft.at[top], x_right), (lft, mate), (rgt.at[bot], x_left), (rgt, mate),
            (far.at[top], mate), (far.at[bot], mate),
        )
        return [remote(r, r, ag_send.at[k, i], ag_recv.at[k, i], dev) for i, (r, dev) in enumerate(plan)]

    def ag_lands(act, k):
        o = 1 - c
        top, bot = pl.ds(0, half), pl.ds(half, half)
        far, ofar = act.at[2 * x2 + c], act.at[2 * x2 + o]
        plan = (
            act.at[2 * xl + c], act.at[2 * xr + c], act.at[2 * x + o],
            far.at[top], act.at[2 * xl + o], far.at[bot], act.at[2 * xr + o],
            ofar.at[top], ofar.at[bot],
        )
        return [remote(r, r, ag_send.at[k, i], ag_recv.at[k, i], mate) for i, r in enumerate(plan)]

    def rs_copies(k, terms, mt, turn, fin):
        top, bot = pl.ds(0, half), pl.ds(half, half)
        plan = [(terms.at[2 * v + 1 - c], mt.at[v], mate) for v in (x2, xr, xl, x)]
        plan += [
            (terms.at[2 * x2 + c, top], turn.at[0], x_right),
            (terms.at[2 * x2 + c, bot], turn.at[1], x_left),
            (terms.at[2 * xr + c, bot], fin.at[0, bot], x_right),
            (terms.at[2 * xl + c, top], fin.at[1, top], x_left),
            (terms.at[2 * xr + c, top], fin.at[0, top], x_right),
            (terms.at[2 * xl + c, bot], fin.at[1, bot], x_left),
        ]
        return [remote(s, d, rs_send.at[k, i], rs_recv.at[k, i], dev) for i, (s, d, dev) in enumerate(plan)]

    def reduce_scatter(k, term_of, terms, mt, turn, fin, between):
        copies = rs_copies(k, terms, mt, turn, fin)
        top, bot = pl.ds(0, half), pl.ds(half, half)
        for i, v in enumerate((x2, xr, xl, x)):
            terms[2 * v + 1 - c] = term_of(2 * v + 1 - c).astype(BF16)
            copies[i].start()
            terms[2 * v + c] = term_of(2 * v + c).astype(BF16)

        def join(i, v):
            copies[i].wait_recv()
            terms[2 * v + c] = (terms[2 * v + c].astype(F32) + mt[v].astype(F32)).astype(BF16)

        join(0, x2)
        copies[4].start()
        copies[5].start()
        join(1, xr)
        copies[6].start()
        join(2, xl)
        copies[7].start()
        between()
        copies[4].wait_recv()
        terms[2 * xr + c, top] = (terms[2 * xr + c, top].astype(F32) + turn[0].astype(F32)).astype(BF16)
        copies[8].start()
        copies[5].wait_recv()
        terms[2 * xl + c, bot] = (terms[2 * xl + c, bot].astype(F32) + turn[1].astype(F32)).astype(BF16)
        copies[9].start()
        copies[3].wait_recv()
        total = terms[2 * x + c].astype(F32) + mt[x].astype(F32)
        for i in (6, 7, 8, 9):
            copies[i].wait_recv()
        total += fin[0].astype(F32) + fin[1].astype(F32)
        return total, copies

    def norm(act, gain):
        total = jnp.zeros((rows, 1), F32)
        for b in range(ntp):
            v = act[b].astype(F32)
            total += jnp.sum(v * v, axis=1, keepdims=True)
        scale = lax.rsqrt(total / (ntp * db) + 1e-06)
        for b in range(ntp):
            cols = slice(b * db, (b + 1) * db)
            normed[:, cols] = (act[b].astype(F32) * scale * gain[:, cols]).astype(BF16)

    mine = pl.ds(pl.multiple_of(z * depth, depth), depth)
    for k, ref in enumerate((w_sig, w_out, w_inn, w_mo)):
        gm[c, k, mine, :] = ref[...]
    act0[t] = tok[...]
    for b in range(nf):
        cols = slice(b * LANES, (b + 1) * LANES)
        gg[c, b, mine, :] = w_gate[:, cols]
        gg[c, nf + b, mine, :] = w_val[:, cols]
        gd[c, b, mine, :] = w_down[:, cols]

    barrier = pltpu.get_barrier_semaphore()
    near = (x_right, x_left, mate, {"grp": other}, {"grp": other, "tp": 2 * x + 1 - c})
    below = [{"fs": lax.rem(z + nz - k, nz)} for k in (1, 2)]
    above = [{"fs": lax.rem(z + k, nz)} for k in (1, 2)]
    for dev in (*below, *above, *near):
        pl.semaphore_signal(barrier, inc=1, device_id=dev, device_id_type=MESH)
    pl.semaphore_wait(barrier, len(near) + len(above) + len(below))

    names = ("m", "g", "d")
    to_mate = []
    for i, name in enumerate(names):
        p = z_part(name, 0 if name == "m" else 1, z)
        to_mate.append(remote(p, p, own_send.at[i], own_recv.at[i], mate))
    ag0, land0 = ag_copies(act0, 0), ag_lands(act0, 0)

    @pl.when(is_f)
    def _():
        to_mate[0].start()
        open_ring("f", (0,))

    @pl.when(is_m)
    def _():
        to_mate[1].start()
        to_mate[2].start()
        open_ring("m", (1,))
        to_mate[0].wait_recv()
        open_ring("m", (0,))

    for i in (0, 1, 2):
        ag0[i].start()

    @pl.when(is_f)
    def _():
        to_mate[1].wait_recv()
        to_mate[2].wait_recv()
        open_ring("f", (1,))

    mixer_steps(0, 1)
    bulk_steps(0, 1)
    land0[0].wait_recv()
    ag0[3].start()
    ag0[4].start()
    land0[1].wait_recv()
    ag0[5].start()
    ag0[6].start()
    mixer_steps(1, 2)
    bulk_steps(1, 2)
    land0[3].wait_recv()
    ag0[7].start()
    land0[5].wait_recv()
    ag0[8].start()
    for i in (2, 4, 6, 7, 8):
        land0[i].wait_recv()
    norm(act0, mix_gain)
    mixer_steps(2, mixer_end)
    done = bulk_steps(2, MIXER_AT)
    arrive("m")

    wide = jnp.concatenate([gm[c, 0], gm[c, 1], gm[c, 2]], axis=1)
    three = dot(normed[...], wide).astype(BF16).astype(F32)
    signal, outer, inner = (three[:, k * LANES : (k + 1) * LANES] for k in range(3))
    mixed = (outer * conv_positions(inner * signal, mix_taps[...], length)).astype(BF16)

    done = bulk_steps(done, done + 1)

    def mix_term(b):
        return dot_nt(mixed, gm[c, 3, pl.ds(pl.multiple_of(b * db, db), db), :])

    total, rs0 = reduce_scatter(0, mix_term, terms0, mate0, turn0, fin0, lambda: None)
    stream = (tok[...].astype(F32) + total).astype(BF16)
    resid[...] = stream
    act1[t] = stream
    ag1, land1 = ag_copies(act1, 1), ag_lands(act1, 1)
    for i in (0, 1, 2):
        ag1[i].start()
    done = bulk_steps(done, done + 2)
    land1[0].wait_recv()
    ag1[3].start()
    ag1[4].start()
    land1[1].wait_recv()
    ag1[5].start()
    ag1[6].start()
    done = bulk_steps(done, done + 1)
    land1[3].wait_recv()
    ag1[7].start()
    land1[5].wait_recv()
    ag1[8].start()
    done = bulk_steps(done, done + 1)
    for i in (2, 4, 6, 7, 8):
        land1[i].wait_recv()
    norm(act1, ffn_gain)
    bulk_steps(done, bulk_end)

    arrive("g")
    for b in range(nf):
        both = dot(normed[...], jnp.concatenate([gg[c, b], gg[c, nf + b]], axis=1)).astype(BF16).astype(F32)
        cols = slice(b * LANES, (b + 1) * LANES)
        gate = conv_positions(both[:, :LANES], up_taps[:, 0, cols], length) + up_bias[0:1, cols]
        value = conv_positions(both[:, LANES:], up_taps[:, 1, cols], length) + up_bias[1:2, cols]
        hidden[:, cols] = (gate / (1.0 + jnp.exp(-gate)) * value).astype(BF16)
    arrive("d")

    def ffn_term(b):
        at = pl.ds(pl.multiple_of(b * db, db), db)
        return dot_nt(hidden[...], jnp.concatenate([gd[c, i, at, :] for i in range(nf)], axis=1))

    total, rs1 = reduce_scatter(1, ffn_term, terms1, mate1, turn1, fin1, lambda: None)
    out[...] = (resid[...].astype(F32) + total).astype(BF16)

    for copy in (*ag0, *ag1, *rs0, *rs1):
        copy.wait_send()

    def drain(name):
        k, n, span = index[name], ONE[name] + BOTH[name], pl.ds(0, (nz - 1) * depth)
        sent = refs[name].at[:, pl.ds(0, n), span, :]
        remote(sent, sent, ring_send.at[k], own_recv.at[0], mate).wait_send()
        crossed = refs[name].at[:, pl.ds(0, ONE[name]), span, :]
        remote(crossed, crossed, y_send.at[k], own_recv.at[0], mate).wait_send()
        pushed = refs[name].at[0, pl.ds(0, n), span, :]
        remote(pushed, pushed, push_send.at[k], own_recv.at[0], mate).wait_send()

    @pl.when(is_f)
    def _():
        to_mate[0].wait_send()
        drain("g")
        drain("d")

    @pl.when(is_m)
    def _():
        to_mate[1].wait_send()
        to_mate[2].wait_send()
        drain("m")


def on_device(sizes, tokens, mix_gain, w_signal, w_outer, w_inner, mix_taps, w_mix_out, ffn_gain, w_gate, w_value, up_taps, up_bias, w_down):
    rows, db = tokens.shape
    ntp, nz = sizes[2], sizes[1]
    d = ntp * db
    nf = w_gate.shape[1] // LANES
    half = rows // 2
    vmem, dma = pltpu.VMEM, pltpu.SemaphoreType.DMA
    act = vmem((ntp, rows, db), BF16)
    mt, turn, fin = vmem((ntp // 2, rows, db), BF16), vmem((2, half, db), BF16), vmem((2, rows, db), BF16)
    scratch = [
        vmem((2, 4, d, LANES), BF16), vmem((2, 2 * nf, d, LANES), BF16), vmem((2, nf, d, LANES), BF16),
        act, act, vmem((rows, d), BF16), act, act, mt, mt, turn, turn, fin, fin,
        vmem((rows, db), BF16), vmem((rows, nf * LANES), BF16),
        dma((2, 2, nz)), dma((2, 2, nz)), dma((2, 2, nz)), dma((3,)), dma((3,)), dma((3,)), dma((3,)), dma((3,)),
        dma((3,)), dma((3,)), dma((2, 9)), dma((2, 9)), dma((2, 10)), dma((2, 10)),
    ]
    args = (
        tokens, mix_gain.reshape(1, d), w_signal, w_outer, w_inner, mix_taps, w_mix_out.T, ffn_gain.reshape(1, d),
        w_gate, w_value, jnp.transpose(up_taps, (1, 0, 2)), up_bias, w_down.T,
    )
    return pl.pallas_call(
        functools.partial(kernel, sizes),
        out_shape=jax.ShapeDtypeStruct((rows, db), BF16),
        in_specs=[pl.BlockSpec(memory_space=vmem)] * len(args),
        out_specs=pl.BlockSpec(memory_space=vmem),
        scratch_shapes=scratch,
        compiler_params=pltpu.CompilerParams(
            collective_id=0, has_side_effects=True, vmem_limit_bytes=60 * 1024 * 1024
        ),
        name="layer",
    )(*args)


def solution(mesh):
    sizes = (mesh.shape["grp"], mesh.shape["fs"], mesh.shape["tp"])
    placed = (
        P(("grp", "fs"), "tp"), P(), P("fs", "tp"), P("fs", "tp"), P("fs", "tp"), P(None, "tp"), P("tp", "fs"), P(),
        P("fs", "tp"), P("fs", "tp"), P(None, None, "tp"), P(None, "tp"), P("tp", "fs"),
    )
    return jax.shard_map(
        functools.partial(on_device, sizes),
        mesh=mesh, in_specs=placed, out_specs=P(("grp", "fs"), "tp"), check_vma=False,
    )
```

```python
import functools

import jax
import jax.numpy as jnp
from jax import lax
from jax.experimental import pallas as pl
from jax.experimental.pallas import tpu as pltpu
from jax.sharding import PartitionSpec as P

SEQS_DEV = 2
LANES = 128
MESH = pl.DeviceIdType.MESH
F32, BF16 = jnp.float32, jnp.bfloat16

ONE = {"m": 2, "g": 4, "d": 1}
BOTH = {"m": 0, "g": 2, "d": 3}
UP_M, UP_F = 16, 16
MIXER_AT = 11


def conv_positions(values, taps, length):
    row = lax.rem(lax.broadcasted_iota(jnp.int32, values.shape, 0), length)
    back1 = jnp.where(row >= 1, pltpu.roll(values, 1, 0), 0.0)
    back2 = jnp.where(row >= 2, pltpu.roll(values, 2, 0), 0.0)
    return back2 * taps[0:1] + back1 * taps[1:2] + values * taps[2:3]


def dot(a, b):
    return jnp.dot(a, b, preferred_element_type=F32)


def dot_nt(a, b):
    return lax.dot_general(a, b, (((1,), (1,)), ((), ())), preferred_element_type=F32)


def kernel(
    sizes,
    tok, mix_gain, w_sig, w_out, w_inn, mix_taps, w_mo, ffn_gain, w_gate, w_val, up_taps, up_bias, w_down,
    out,
    gm, gg, gd, act0, act1, normed, terms0, terms1, mate0, mate1, turn0, turn1, fin0, fin1, resid, hidden,
    m_recv, g_recv, d_recv, ring_send, y_send, y_recv, push_send, push_recv, own_send, own_recv,
    ag_send, ag_recv, rs_send, rs_recv,
):
    ngrp, nz, ntp = sizes
    nx = ntp // 2
    rows, db = tok.shape
    half = rows // 2
    length = rows // SEQS_DEV
    depth = w_sig.shape[0]
    nf = w_gate.shape[1] // LANES
    g, z, t = lax.axis_index("grp"), lax.axis_index("fs"), lax.axis_index("tp")
    y, x, c = lax.rem(g, 2), lax.div(t, 2), lax.rem(t, 2)
    other = g + 1 - 2 * y
    xr, xl, x2 = lax.rem(x + 1, nx), lax.rem(x + nx - 1, nx), lax.rem(x + 2, nx)
    x_right, x_left, mate = {"tp": 2 * xr + c}, {"tp": 2 * xl + c}, {"tp": 2 * x + 1 - c}
    def remote(src, dst, ssem, rsem, dev):
        return pltpu.make_async_remote_copy(
            src_ref=src, dst_ref=dst, send_sem=ssem, recv_sem=rsem, device_id=dev, device_id_type=MESH
        )

    refs = {"m": gm, "g": gg, "d": gd}
    index = {"m": 0, "g": 1, "d": 2}
    most = {"m": (UP_M, nz - 1 - UP_M), "g": (UP_F, nz - 1 - UP_F), "d": (UP_F, nz - 1 - UP_F)}
    recv_of = {"m": m_recv, "g": g_recv, "d": d_recv}
    is_m, is_f = c == 1, c == 0

    def z_part(name, col, origin):
        at = pl.ds(pl.multiple_of(origin * depth, depth), depth)
        return refs[name].at[col, pl.ds(ONE[name] * y, ONE[name] + BOTH[name]), at, :]

    def y_part(name, col, origin):
        at = pl.ds(pl.multiple_of(origin * depth, depth), depth)
        return refs[name].at[col, pl.ds((ONE[name] + BOTH[name]) * y, ONE[name]), at, :]

    def fs_at(k):
        return lax.rem(z + nz + k, nz)

    def origin_of(way, dist):
        return fs_at(-dist if way == 0 else dist)

    def send(name, col, way, dist, hops):
        part = z_part(name, col, origin_of(way, dist))
        to = {"fs": fs_at(hops if way == 0 else -hops)}
        remote(part, part, ring_send.at[index[name]], recv_of[name].at[col, way, dist + hops - 1], to).start()

    def landed(name, col, way, dist):
        part = z_part(name, col, origin_of(way, dist))
        sem = recv_of[name].at[col, way, dist - 1]
        remote(part, part, ring_send.at[index[name]], sem, mate).wait_recv()

    def spread(name, col, way, dist):
        k, origin = index[name], origin_of(way, dist)
        part, cross = z_part(name, col, origin), y_part(name, col, origin)
        remote(cross, cross, y_send.at[k], y_recv.at[k], {"grp": other, "tp": 2 * x + col}).start()
        if col != (1 if name == "m" else 0):
            remote(part, part, push_send.at[k], push_recv.at[k], mate).start()

    def mixer_step(i):
        dist = i + 1
        for col in (0, 1):
            for way in (0, 1):
                @pl.when(dist <= most["m"][way])
                def _(way=way):
                    landed("m", col, way, dist)
                    pl.when(dist + 1 <= most["m"][way])(lambda: send("m", col, way, dist, 1))
                    spread("m", col, way, dist)

    def bulk_step(i):
        dist = i + 1
        for col in (0, 1):
            for name in ("g", "d"):
                for way in (0, 1):
                    @pl.when(dist <= most[name][way])
                    def _(way=way):
                        landed(name, col, way, dist)
                        pl.when(dist + 1 <= most[name][way])(lambda: send(name, col, way, dist, 1))
                        spread(name, col, way, dist)

    def open_ring(kind, cols):
        for col in cols:
            for way in (0, 1):
                if kind == "m":
                    send("m", col, way, 0, 1)
                else:
                    for name in ("g", "d"):
                        send(name, col, way, 0, 1)

    mixer_end = max(most["m"])
    bulk_end = max(most["g"])

    def mixer_steps(lo, hi):
        def body(i, _):
            mixer_step(i)
            return 0

        lax.fori_loop(lo, jnp.where(is_m, hi, lo), body, 0)

    def bulk_steps(lo, hi):
        hi = min(hi, bulk_end)
        lax.fori_loop(lo, jnp.where(is_f, hi, lo), lambda i, _: (bulk_step(i), 0)[1], 0)
        return hi

    def arrive(name):
        k, span = index[name], pl.ds(0, (nz - 1) * depth)
        part = refs[name].at[0, pl.ds(0, ONE[name]), span, :]
        remote(part, part, y_send.at[k], y_recv.at[k], mate).wait_recv()
        rest = refs[name].at[0, pl.ds(0, ONE[name] + BOTH[name]), span, :]
        pl.when(is_f if name == "m" else is_m)(
            lambda: remote(rest, rest, push_send.at[k], push_recv.at[k], mate).wait_recv()
        )

    def ag_copies(act, k):
        own, lft, rgt, far = act.at[t], act.at[2 * xl + c], act.at[2 * xr + c], act.at[2 * x2 + c]
        top, bot = pl.ds(0, half), pl.ds(half, half)
        plan = (
            (own, x_right), (own, x_left), (own, mate),
            (lft.at[top], x_right), (lft, mate), (rgt.at[bot], x_left), (rgt, mate),
            (far.at[top], mate), (far.at[bot], mate),
        )
        return [remote(r, r, ag_send.at[k, i], ag_recv.at[k, i], dev) for i, (r, dev) in enumerate(plan)]

    def ag_lands(act, k):
        o = 1 - c
        top, bot = pl.ds(0, half), pl.ds(half, half)
        far, ofar = act.at[2 * x2 + c], act.at[2 * x2 + o]
        plan = (
            act.at[2 * xl + c], act.at[2 * xr + c], act.at[2 * x + o],
            far.at[top], act.at[2 * xl + o], far.at[bot], act.at[2 * xr + o],
            ofar.at[top], ofar.at[bot],
        )
        return [remote(r, r, ag_send.at[k, i], ag_recv.at[k, i], mate) for i, r in enumerate(plan)]

    def rs_copies(k, terms, mt, turn, fin):
        top, bot = pl.ds(0, half), pl.ds(half, half)
        plan = [(terms.at[2 * v + 1 - c], mt.at[v], mate) for v in (x2, xr, xl, x)]
        plan += [
            (terms.at[2 * x2 + c, top], turn.at[0], x_right),
            (terms.at[2 * x2 + c, bot], turn.at[1], x_left),
            (terms.at[2 * xr + c, bot], fin.at[0, bot], x_right),
            (terms.at[2 * xl + c, top], fin.at[1, top], x_left),
            (terms.at[2 * xr + c, top], fin.at[0, top], x_right),
            (terms.at[2 * xl + c, bot], fin.at[1, bot], x_left),
        ]
        return [remote(s, d, rs_send.at[k, i], rs_recv.at[k, i], dev) for i, (s, d, dev) in enumerate(plan)]

    def reduce_scatter(k, term_of, terms, mt, turn, fin, between):
        copies = rs_copies(k, terms, mt, turn, fin)
        top, bot = pl.ds(0, half), pl.ds(half, half)
        for i, v in enumerate((x2, xr, xl, x)):
            terms[2 * v + 1 - c] = term_of(2 * v + 1 - c).astype(BF16)
            copies[i].start()
            terms[2 * v + c] = term_of(2 * v + c).astype(BF16)

        def join(i, v):
            copies[i].wait_recv()
            terms[2 * v + c] = (terms[2 * v + c].astype(F32) + mt[v].astype(F32)).astype(BF16)

        join(0, x2)
        copies[4].start()
        copies[5].start()
        join(1, xr)
        copies[6].start()
        join(2, xl)
        copies[7].start()
        between()
        copies[4].wait_recv()
        terms[2 * xr + c, top] = (terms[2 * xr + c, top].astype(F32) + turn[0].astype(F32)).astype(BF16)
        copies[8].start()
        copies[5].wait_recv()
        terms[2 * xl + c, bot] = (terms[2 * xl + c, bot].astype(F32) + turn[1].astype(F32)).astype(BF16)
        copies[9].start()
        copies[3].wait_recv()
        total = terms[2 * x + c].astype(F32) + mt[x].astype(F32)
        for i in (6, 7, 8, 9):
            copies[i].wait_recv()
        total += fin[0].astype(F32) + fin[1].astype(F32)
        return total, copies

    def norm(act, gain):
        total = jnp.zeros((rows, 1), F32)
        for b in range(ntp):
            v = act[b].astype(F32)
            total += jnp.sum(v * v, axis=1, keepdims=True)
        scale = lax.rsqrt(total / (ntp * db) + 1e-06)
        for b in range(ntp):
            cols = slice(b * db, (b + 1) * db)
            normed[:, cols] = (act[b].astype(F32) * scale * gain[:, cols]).astype(BF16)

    mine = pl.ds(pl.multiple_of(z * depth, depth), depth)
    for k, ref in enumerate((w_sig, w_out, w_inn, w_mo)):
        gm[c, k, mine, :] = ref[...]
    act0[t] = tok[...]
    for b in range(nf):
        cols = slice(b * LANES, (b + 1) * LANES)
        gg[c, b, mine, :] = w_gate[:, cols]
        gg[c, nf + b, mine, :] = w_val[:, cols]
        gd[c, b, mine, :] = w_down[:, cols]

    barrier = pltpu.get_barrier_semaphore()
    near = (x_right, x_left, mate, {"grp": other}, {"grp": other, "tp": 2 * x + 1 - c})
    below = [{"fs": lax.rem(z + nz - k, nz)} for k in (1, 2)]
    above = [{"fs": lax.rem(z + k, nz)} for k in (1, 2)]
    for dev in (*below, *above, *near):
        pl.semaphore_signal(barrier, inc=1, device_id=dev, device_id_type=MESH)
    pl.semaphore_wait(barrier, len(near) + len(above) + len(below))

    names = ("m", "g", "d")
    to_mate = []
    for i, name in enumerate(names):
        p = z_part(name, 0 if name == "m" else 1, z)
        to_mate.append(remote(p, p, own_send.at[i], own_recv.at[i], mate))
    ag0, land0 = ag_copies(act0, 0), ag_lands(act0, 0)

    @pl.when(is_f)
    def _():
        to_mate[0].start()
        open_ring("f", (0,))

    @pl.when(is_m)
    def _():
        to_mate[1].start()
        to_mate[2].start()
        open_ring("m", (1,))
        to_mate[0].wait_recv()
        open_ring("m", (0,))

    for i in (0, 1, 2):
        ag0[i].start()

    @pl.when(is_f)
    def _():
        to_mate[1].wait_recv()
        to_mate[2].wait_recv()
        open_ring("f", (1,))

    mixer_steps(0, 1)
    bulk_steps(0, 1)
    land0[0].wait_recv()
    ag0[3].start()
    ag0[4].start()
    land0[1].wait_recv()
    ag0[5].start()
    ag0[6].start()
    mixer_steps(1, 2)
    bulk_steps(1, 2)
    land0[3].wait_recv()
    ag0[7].start()
    land0[5].wait_recv()
    ag0[8].start()
    for i in (2, 4, 6, 7, 8):
        land0[i].wait_recv()
    norm(act0, mix_gain)
    mixer_steps(2, mixer_end)
    done = bulk_steps(2, MIXER_AT)
    arrive("m")

    wide = jnp.concatenate([gm[c, 0], gm[c, 1], gm[c, 2]], axis=1)
    three = dot(normed[...], wide).astype(BF16).astype(F32)
    signal, outer, inner = (three[:, k * LANES : (k + 1) * LANES] for k in range(3))
    mixed = (outer * conv_positions(inner * signal, mix_taps[...], length)).astype(BF16)

    done = bulk_steps(done, done + 1)

    def mix_term(b):
        return dot_nt(mixed, gm[c, 3, pl.ds(pl.multiple_of(b * db, db), db), :])

    total, rs0 = reduce_scatter(0, mix_term, terms0, mate0, turn0, fin0, lambda: None)
    stream = (tok[...].astype(F32) + total).astype(BF16)
    resid[...] = stream
    act1[t] = stream
    ag1, land1 = ag_copies(act1, 1), ag_lands(act1, 1)
    for i in (0, 1, 2):
        ag1[i].start()
    done = bulk_steps(done, done + 2)
    land1[0].wait_recv()
    ag1[3].start()
    ag1[4].start()
    land1[1].wait_recv()
    ag1[5].start()
    ag1[6].start()
    done = bulk_steps(done, done + 1)
    land1[3].wait_recv()
    ag1[7].start()
    land1[5].wait_recv()
    ag1[8].start()
    done = bulk_steps(done, done + 1)
    for i in (2, 4, 6, 7, 8):
        land1[i].wait_recv()
    norm(act1, ffn_gain)
    bulk_steps(done, bulk_end)

    arrive("g")
    for b in range(nf):
        both = dot(normed[...], jnp.concatenate([gg[c, b], gg[c, nf + b]], axis=1)).astype(BF16).astype(F32)
        cols = slice(b * LANES, (b + 1) * LANES)
        gate = conv_positions(both[:, :LANES], up_taps[:, 0, cols], length) + up_bias[0:1, cols]
        value = conv_positions(both[:, LANES:], up_taps[:, 1, cols], length) + up_bias[1:2, cols]
        hidden[:, cols] = (gate / (1.0 + jnp.exp(-gate)) * value).astype(BF16)
    arrive("d")

    def ffn_term(b):
        at = pl.ds(pl.multiple_of(b * db, db), db)
        return dot_nt(hidden[...], jnp.concatenate([gd[c, i, at, :] for i in range(nf)], axis=1))

    total, rs1 = reduce_scatter(1, ffn_term, terms1, mate1, turn1, fin1, lambda: None)
    out[...] = (resid[...].astype(F32) + total).astype(BF16)

    for copy in (*ag0, *ag1, *rs0, *rs1):
        copy.wait_send()

    def drain(name):
        k, n, span = index[name], ONE[name] + BOTH[name], pl.ds(0, (nz - 1) * depth)
        sent = refs[name].at[:, pl.ds(0, n), span, :]
        remote(sent, sent, ring_send.at[k], own_recv.at[0], mate).wait_send()
        crossed = refs[name].at[:, pl.ds(0, ONE[name]), span, :]
        remote(crossed, crossed, y_send.at[k], own_recv.at[0], mate).wait_send()
        pushed = refs[name].at[0, pl.ds(0, n), span, :]
        remote(pushed, pushed, push_send.at[k], own_recv.at[0], mate).wait_send()

    @pl.when(is_f)
    def _():
        to_mate[0].wait_send()
        drain("g")
        drain("d")

    @pl.when(is_m)
    def _():
        to_mate[1].wait_send()
        to_mate[2].wait_send()
        drain("m")


def on_device(sizes, tokens, mix_gain, w_signal, w_outer, w_inner, mix_taps, w_mix_out, ffn_gain, w_gate, w_value, up_taps, up_bias, w_down):
    rows, db = tokens.shape
    ntp, nz = sizes[2], sizes[1]
    d = ntp * db
    nf = w_gate.shape[1] // LANES
    half = rows // 2
    vmem, dma = pltpu.VMEM, pltpu.SemaphoreType.DMA
    act = vmem((ntp, rows, db), BF16)
    mt, turn, fin = vmem((ntp // 2, rows, db), BF16), vmem((2, half, db), BF16), vmem((2, rows, db), BF16)
    scratch = [
        vmem((2, 4, d, LANES), BF16), vmem((2, 2 * nf, d, LANES), BF16), vmem((2, nf, d, LANES), BF16),
        act, act, vmem((rows, d), BF16), act, act, mt, mt, turn, turn, fin, fin,
        vmem((rows, db), BF16), vmem((rows, nf * LANES), BF16),
        dma((2, 2, nz)), dma((2, 2, nz)), dma((2, 2, nz)), dma((3,)), dma((3,)), dma((3,)), dma((3,)), dma((3,)),
        dma((3,)), dma((3,)), dma((2, 9)), dma((2, 9)), dma((2, 10)), dma((2, 10)),
    ]
    args = (
        tokens, mix_gain.reshape(1, d), w_signal, w_outer, w_inner, mix_taps, w_mix_out.T, ffn_gain.reshape(1, d),
        w_gate, w_value, jnp.transpose(up_taps, (1, 0, 2)), up_bias, w_down.T,
    )
    return pl.pallas_call(
        functools.partial(kernel, sizes),
        out_shape=jax.ShapeDtypeStruct((rows, db), BF16),
        in_specs=[pl.BlockSpec(memory_space=vmem)] * len(args),
        out_specs=pl.BlockSpec(memory_space=vmem),
        scratch_shapes=scratch,
        compiler_params=pltpu.CompilerParams(
            collective_id=0, has_side_effects=True, vmem_limit_bytes=60 * 1024 * 1024
        ),
        name="layer",
    )(*args)


def solution(mesh):
    sizes = (mesh.shape["grp"], mesh.shape["fs"], mesh.shape["tp"])
    placed = (
        P(("grp", "fs"), "tp"), P(), P("fs", "tp"), P("fs", "tp"), P("fs", "tp"), P(None, "tp"), P("tp", "fs"), P(),
        P("fs", "tp"), P("fs", "tp"), P(None, None, "tp"), P(None, "tp"), P("tp", "fs"),
    )
    return jax.shard_map(
        functools.partial(on_device, sizes),
        mesh=mesh, in_specs=placed, out_specs=P(("grp", "fs"), "tp"), check_vma=False,
    )
```

```python
import functools

import jax
import jax.numpy as jnp
from jax import lax
from jax.experimental import pallas as pl
from jax.experimental.pallas import tpu as pltpu
from jax.sharding import PartitionSpec as P

SEQS_DEV = 2
LANES = 128
MESH = pl.DeviceIdType.MESH
F32, BF16 = jnp.float32, jnp.bfloat16

ONE = {"m": 2, "g": 4, "d": 1}
BOTH = {"m": 0, "g": 2, "d": 3}
UP_M, UP_F = 16, 16
MIXER_AT = 11


def conv_positions(values, taps, length):
    row = lax.rem(lax.broadcasted_iota(jnp.int32, values.shape, 0), length)
    back1 = jnp.where(row >= 1, pltpu.roll(values, 1, 0), 0.0)
    back2 = jnp.where(row >= 2, pltpu.roll(values, 2, 0), 0.0)
    return back2 * taps[0:1] + back1 * taps[1:2] + values * taps[2:3]


def dot(a, b):
    return jnp.dot(a, b, preferred_element_type=F32)


def dot_nt(a, b):
    return lax.dot_general(a, b, (((1,), (1,)), ((), ())), preferred_element_type=F32)


def kernel(
    sizes,
    tok, mix_gain, w_sig, w_out, w_inn, mix_taps, w_mo, ffn_gain, w_gate, w_val, up_taps, up_bias, w_down,
    out,
    gm, gg, gd, act0, act1, normed, terms0, terms1, mate0, mate1, turn0, turn1, fin0, fin1, resid, hidden,
    m_recv, g_recv, d_recv, ring_send, y_send, y_recv, push_send, push_recv, own_send, own_recv,
    ag_send, ag_recv, rs_send, rs_recv,
):
    ngrp, nz, ntp = sizes
    nx = ntp // 2
    rows, db = tok.shape
    half = rows // 2
    length = rows // SEQS_DEV
    depth = w_sig.shape[0]
    nf = w_gate.shape[1] // LANES
    g, z, t = lax.axis_index("grp"), lax.axis_index("fs"), lax.axis_index("tp")
    y, x, c = lax.rem(g, 2), lax.div(t, 2), lax.rem(t, 2)
    other = g + 1 - 2 * y
    xr, xl, x2 = lax.rem(x + 1, nx), lax.rem(x + nx - 1, nx), lax.rem(x + 2, nx)
    x_right, x_left, mate = {"tp": 2 * xr + c}, {"tp": 2 * xl + c}, {"tp": 2 * x + 1 - c}
    def remote(src, dst, ssem, rsem, dev):
        return pltpu.make_async_remote_copy(
            src_ref=src, dst_ref=dst, send_sem=ssem, recv_sem=rsem, device_id=dev, device_id_type=MESH
        )

    refs = {"m": gm, "g": gg, "d": gd}
    index = {"m": 0, "g": 1, "d": 2}
    most = {"m": (UP_M, nz - 1 - UP_M), "g": (UP_F, nz - 1 - UP_F), "d": (UP_F, nz - 1 - UP_F)}
    recv_of = {"m": m_recv, "g": g_recv, "d": d_recv}
    is_m, is_f = c == 1, c == 0

    def z_part(name, col, origin):
        at = pl.ds(pl.multiple_of(origin * depth, depth), depth)
        return refs[name].at[col, pl.ds(ONE[name] * y, ONE[name] + BOTH[name]), at, :]

    def y_part(name, col, origin):
        at = pl.ds(pl.multiple_of(origin * depth, depth), depth)
        return refs[name].at[col, pl.ds((ONE[name] + BOTH[name]) * y, ONE[name]), at, :]

    def fs_at(k):
        return lax.rem(z + nz + k, nz)

    def origin_of(way, dist):
        return fs_at(-dist if way == 0 else dist)

    def send(name, col, way, dist, hops):
        part = z_part(name, col, origin_of(way, dist))
        to = {"fs": fs_at(hops if way == 0 else -hops)}
        remote(part, part, ring_send.at[index[name]], recv_of[name].at[col, way, dist + hops - 1], to).start()

    def landed(name, col, way, dist):
        part = z_part(name, col, origin_of(way, dist))
        sem = recv_of[name].at[col, way, dist - 1]
        remote(part, part, ring_send.at[index[name]], sem, mate).wait_recv()

    def spread(name, col, way, dist):
        k, origin = index[name], origin_of(way, dist)
        part, cross = z_part(name, col, origin), y_part(name, col, origin)
        remote(cross, cross, y_send.at[k], y_recv.at[k], {"grp": other, "tp": 2 * x + col}).start()
        if col != (1 if name == "m" else 0):
            remote(part, part, push_send.at[k], push_recv.at[k], mate).start()

    def mixer_step(i):
        dist = i + 1
        for col in (0, 1):
            for way in (0, 1):
                @pl.when(dist <= most["m"][way])
                def _(way=way):
                    landed("m", col, way, dist)
                    pl.when(dist + 1 <= most["m"][way])(lambda: send("m", col, way, dist, 1))
                    spread("m", col, way, dist)

    def bulk_step(i):
        dist = i + 1
        for col in (0, 1):
            for name in ("g", "d"):
                for way in (0, 1):
                    @pl.when(dist <= most[name][way])
                    def _(way=way):
                        landed(name, col, way, dist)
                        pl.when(dist + 1 <= most[name][way])(lambda: send(name, col, way, dist, 1))
                        spread(name, col, way, dist)

    def open_ring(kind, cols):
        for col in cols:
            for way in (0, 1):
                if kind == "m":
                    send("m", col, way, 0, 1)
                else:
                    for name in ("g", "d"):
                        send(name, col, way, 0, 1)

    mixer_end = max(most["m"])
    bulk_end = max(most["g"])

    def mixer_steps(lo, hi):
        def body(i, _):
            mixer_step(i)
            return 0

        lax.fori_loop(lo, jnp.where(is_m, hi, lo), body, 0)

    def bulk_steps(lo, hi):
        hi = min(hi, bulk_end)
        lax.fori_loop(lo, jnp.where(is_f, hi, lo), lambda i, _: (bulk_step(i), 0)[1], 0)
        return hi

    def arrive(name):
        k, span = index[name], pl.ds(0, (nz - 1) * depth)
        part = refs[name].at[0, pl.ds(0, ONE[name]), span, :]
        remote(part, part, y_send.at[k], y_recv.at[k], mate).wait_recv()
        rest = refs[name].at[0, pl.ds(0, ONE[name] + BOTH[name]), span, :]
        pl.when(is_f if name == "m" else is_m)(
            lambda: remote(rest, rest, push_send.at[k], push_recv.at[k], mate).wait_recv()
        )

    def ag_copies(act, k):
        own, lft, rgt, far = act.at[t], act.at[2 * xl + c], act.at[2 * xr + c], act.at[2 * x2 + c]
        top, bot = pl.ds(0, half), pl.ds(half, half)
        plan = (
            (own, x_right), (own, x_left), (own, mate),
            (lft.at[top], x_right), (lft, mate), (rgt.at[bot], x_left), (rgt, mate),
            (far.at[top], mate), (far.at[bot], mate),
        )
        return [remote(r, r, ag_send.at[k, i], ag_recv.at[k, i], dev) for i, (r, dev) in enumerate(plan)]

    def ag_lands(act, k):
        o = 1 - c
        top, bot = pl.ds(0, half), pl.ds(half, half)
        far, ofar = act.at[2 * x2 + c], act.at[2 * x2 + o]
        plan = (
            act.at[2 * xl + c], act.at[2 * xr + c], act.at[2 * x + o],
            far.at[top], act.at[2 * xl + o], far.at[bot], act.at[2 * xr + o],
            ofar.at[top], ofar.at[bot],
        )
        return [remote(r, r, ag_send.at[k, i], ag_recv.at[k, i], mate) for i, r in enumerate(plan)]

    def rs_copies(k, terms, mt, turn, fin):
        top, bot = pl.ds(0, half), pl.ds(half, half)
        plan = [(terms.at[2 * v + 1 - c], mt.at[v], mate) for v in (x2, xr, xl, x)]
        plan += [
            (terms.at[2 * x2 + c, top], turn.at[0], x_right),
            (terms.at[2 * x2 + c, bot], turn.at[1], x_left),
            (terms.at[2 * xr + c, bot], fin.at[0, bot], x_right),
            (terms.at[2 * xl + c, top], fin.at[1, top], x_left),
            (terms.at[2 * xr + c, top], fin.at[0, top], x_right),
            (terms.at[2 * xl + c, bot], fin.at[1, bot], x_left),
        ]
        return [remote(s, d, rs_send.at[k, i], rs_recv.at[k, i], dev) for i, (s, d, dev) in enumerate(plan)]

    def reduce_scatter(k, term_of, terms, mt, turn, fin, between):
        copies = rs_copies(k, terms, mt, turn, fin)
        top, bot = pl.ds(0, half), pl.ds(half, half)
        for i, v in enumerate((x2, xr, xl, x)):
            terms[2 * v + 1 - c] = term_of(2 * v + 1 - c).astype(BF16)
            copies[i].start()
            terms[2 * v + c] = term_of(2 * v + c).astype(BF16)

        def join(i, v):
            copies[i].wait_recv()
            terms[2 * v + c] = (terms[2 * v + c].astype(F32) + mt[v].astype(F32)).astype(BF16)

        join(0, x2)
        copies[4].start()
        copies[5].start()
        join(1, xr)
        copies[6].start()
        join(2, xl)
        copies[7].start()
        between()
        copies[4].wait_recv()
        terms[2 * xr + c, top] = (terms[2 * xr + c, top].astype(F32) + turn[0].astype(F32)).astype(BF16)
        copies[8].start()
        copies[5].wait_recv()
        terms[2 * xl + c, bot] = (terms[2 * xl + c, bot].astype(F32) + turn[1].astype(F32)).astype(BF16)
        copies[9].start()
        copies[3].wait_recv()
        total = terms[2 * x + c].astype(F32) + mt[x].astype(F32)
        for i in (6, 7, 8, 9):
            copies[i].wait_recv()
        total += fin[0].astype(F32) + fin[1].astype(F32)
        return total, copies

    def norm(act, gain):
        total = jnp.zeros((rows, 1), F32)
        for b in range(ntp):
            v = act[b].astype(F32)
            total += jnp.sum(v * v, axis=1, keepdims=True)
        scale = lax.rsqrt(total / (ntp * db) + 1e-06)
        for b in range(ntp):
            cols = slice(b * db, (b + 1) * db)
            normed[:, cols] = (act[b].astype(F32) * scale * gain[:, cols]).astype(BF16)

    mine = pl.ds(pl.multiple_of(z * depth, depth), depth)
    for k, ref in enumerate((w_sig, w_out, w_inn, w_mo)):
        gm[c, k, mine, :] = ref[...]
    act0[t] = tok[...]
    for b in range(nf):
        cols = slice(b * LANES, (b + 1) * LANES)
        gg[c, b, mine, :] = w_gate[:, cols]
        gg[c, nf + b, mine, :] = w_val[:, cols]
        gd[c, b, mine, :] = w_down[:, cols]

    barrier = pltpu.get_barrier_semaphore()
    near = (x_right, x_left, mate, {"grp": other}, {"grp": other, "tp": 2 * x + 1 - c})
    below = [{"fs": lax.rem(z + nz - k, nz)} for k in (1, 2)]
    above = [{"fs": lax.rem(z + k, nz)} for k in (1, 2)]
    for dev in (*below, *above, *near):
        pl.semaphore_signal(barrier, inc=1, device_id=dev, device_id_type=MESH)
    pl.semaphore_wait(barrier, len(near) + len(above) + len(below))

    names = ("m", "g", "d")
    to_mate = []
    for i, name in enumerate(names):
        p = z_part(name, 0 if name == "m" else 1, z)
        to_mate.append(remote(p, p, own_send.at[i], own_recv.at[i], mate))
    ag0, land0 = ag_copies(act0, 0), ag_lands(act0, 0)

    @pl.when(is_f)
    def _():
        to_mate[0].start()
        open_ring("f", (0,))

    @pl.when(is_m)
    def _():
        to_mate[1].start()
        to_mate[2].start()
        open_ring("m", (1,))
        to_mate[0].wait_recv()
        open_ring("m", (0,))

    for i in (0, 1, 2):
        ag0[i].start()

    @pl.when(is_f)
    def _():
        to_mate[1].wait_recv()
        to_mate[2].wait_recv()
        open_ring("f", (1,))

    mixer_steps(0, 1)
    bulk_steps(0, 1)
    land0[0].wait_recv()
    ag0[3].start()
    ag0[4].start()
    land0[1].wait_recv()
    ag0[5].start()
    ag0[6].start()
    mixer_steps(1, 2)
    bulk_steps(1, 2)
    land0[3].wait_recv()
    ag0[7].start()
    land0[5].wait_recv()
    ag0[8].start()
    for i in (2, 4, 6, 7, 8):
        land0[i].wait_recv()
    norm(act0, mix_gain)
    mixer_steps(2, mixer_end)
    done = bulk_steps(2, MIXER_AT)
    arrive("m")

    wide = jnp.concatenate([gm[c, 0], gm[c, 1], gm[c, 2]], axis=1)
    three = dot(normed[...], wide).astype(BF16).astype(F32)
    signal, outer, inner = (three[:, k * LANES : (k + 1) * LANES] for k in range(3))
    mixed = (outer * conv_positions(inner * signal, mix_taps[...], length)).astype(BF16)

    def mix_term(b):
        return dot_nt(mixed, gm[c, 3, pl.ds(pl.multiple_of(b * db, db), db), :])

    total, rs0 = reduce_scatter(0, mix_term, terms0, mate0, turn0, fin0, lambda: None)
    stream = (tok[...].astype(F32) + total).astype(BF16)
    resid[...] = stream
    act1[t] = stream
    ag1, land1 = ag_copies(act1, 1), ag_lands(act1, 1)
    for i in (0, 1, 2):
        ag1[i].start()
    done = bulk_steps(done, done + 2)
    land1[0].wait_recv()
    ag1[3].start()
    ag1[4].start()
    land1[1].wait_recv()
    ag1[5].start()
    ag1[6].start()
    done = bulk_steps(done, done + 1)
    land1[3].wait_recv()
    ag1[7].start()
    land1[5].wait_recv()
    ag1[8].start()
    done = bulk_steps(done, done + 1)
    for i in (2, 4, 6, 7, 8):
        land1[i].wait_recv()
    norm(act1, ffn_gain)
    bulk_steps(done, bulk_end)

    arrive("g")
    for b in range(nf):
        both = dot(normed[...], jnp.concatenate([gg[c, b], gg[c, nf + b]], axis=1)).astype(BF16).astype(F32)
        cols = slice(b * LANES, (b + 1) * LANES)
        gate = conv_positions(both[:, :LANES], up_taps[:, 0, cols], length) + up_bias[0:1, cols]
        value = conv_positions(both[:, LANES:], up_taps[:, 1, cols], length) + up_bias[1:2, cols]
        hidden[:, cols] = (gate / (1.0 + jnp.exp(-gate)) * value).astype(BF16)
    arrive("d")

    def ffn_term(b):
        at = pl.ds(pl.multiple_of(b * db, db), db)
        return dot_nt(hidden[...], jnp.concatenate([gd[c, i, at, :] for i in range(nf)], axis=1))

    total, rs1 = reduce_scatter(1, ffn_term, terms1, mate1, turn1, fin1, lambda: None)
    out[...] = (resid[...].astype(F32) + total).astype(BF16)

    for copy in (*ag0, *ag1, *rs0, *rs1):
        copy.wait_send()

    def drain(name):
        k, n, span = index[name], ONE[name] + BOTH[name], pl.ds(0, (nz - 1) * depth)
        sent = refs[name].at[:, pl.ds(0, n), span, :]
        remote(sent, sent, ring_send.at[k], own_recv.at[0], mate).wait_send()
        crossed = refs[name].at[:, pl.ds(0, ONE[name]), span, :]
        remote(crossed, crossed, y_send.at[k], own_recv.at[0], mate).wait_send()
        pushed = refs[name].at[0, pl.ds(0, n), span, :]
        remote(pushed, pushed, push_send.at[k], own_recv.at[0], mate).wait_send()

    @pl.when(is_f)
    def _():
        to_mate[0].wait_send()
        drain("g")
        drain("d")

    @pl.when(is_m)
    def _():
        to_mate[1].wait_send()
        to_mate[2].wait_send()
        drain("m")


def on_device(sizes, tokens, mix_gain, w_signal, w_outer, w_inner, mix_taps, w_mix_out, ffn_gain, w_gate, w_value, up_taps, up_bias, w_down):
    rows, db = tokens.shape
    ntp, nz = sizes[2], sizes[1]
    d = ntp * db
    nf = w_gate.shape[1] // LANES
    half = rows // 2
    vmem, dma = pltpu.VMEM, pltpu.SemaphoreType.DMA
    act = vmem((ntp, rows, db), BF16)
    mt, turn, fin = vmem((ntp // 2, rows, db), BF16), vmem((2, half, db), BF16), vmem((2, rows, db), BF16)
    scratch = [
        vmem((2, 4, d, LANES), BF16), vmem((2, 2 * nf, d, LANES), BF16), vmem((2, nf, d, LANES), BF16),
        act, act, vmem((rows, d), BF16), act, act, mt, mt, turn, turn, fin, fin,
        vmem((rows, db), BF16), vmem((rows, nf * LANES), BF16),
        dma((2, 2, nz)), dma((2, 2, nz)), dma((2, 2, nz)), dma((3,)), dma((3,)), dma((3,)), dma((3,)), dma((3,)),
        dma((3,)), dma((3,)), dma((2, 9)), dma((2, 9)), dma((2, 10)), dma((2, 10)),
    ]
    args = (
        tokens, mix_gain.reshape(1, d), w_signal, w_outer, w_inner, mix_taps, w_mix_out.T, ffn_gain.reshape(1, d),
        w_gate, w_value, jnp.transpose(up_taps, (1, 0, 2)), up_bias, w_down.T,
    )
    return pl.pallas_call(
        functools.partial(kernel, sizes),
        out_shape=jax.ShapeDtypeStruct((rows, db), BF16),
        in_specs=[pl.BlockSpec(memory_space=vmem)] * len(args),
        out_specs=pl.BlockSpec(memory_space=vmem),
        scratch_shapes=scratch,
        compiler_params=pltpu.CompilerParams(
            collective_id=0, has_side_effects=True, vmem_limit_bytes=60 * 1024 * 1024
        ),
        name="layer",
    )(*args)


def solution(mesh):
    sizes = (mesh.shape["grp"], mesh.shape["fs"], mesh.shape["tp"])
    placed = (
        P(("grp", "fs"), "tp"), P(), P("fs", "tp"), P("fs", "tp"), P("fs", "tp"), P(None, "tp"), P("tp", "fs"), P(),
        P("fs", "tp"), P("fs", "tp"), P(None, None, "tp"), P(None, "tp"), P("tp", "fs"),
    )
    return jax.shard_map(
        functools.partial(on_device, sizes),
        mesh=mesh, in_specs=placed, out_specs=P(("grp", "fs"), "tp"), check_vma=False,
    )
```
